256 devices in a mesh: sp: 32 (over z, x), tp: 8 (over y, core).
Axes of the slice: x: 4, y: 4, z: 8, core: 2. Of those that a mesh axis runs over, the one named last changes fastest.
Arguments:
- out_grad: bfloat16 [4096, 2048], P('sp', 'tp'), may hold values from -6 to 6
- moe_input: bfloat16 [4096, 2048], P('sp', 'tp'), may hold values from -6 to 6
- route_weight: float32 [4096, 2], P('sp'), may hold values from 0.2 to 1
- route_ids: int32 [4096, 2], P('sp'), may hold values from 0 to 31, all different within a row; in each aligned block of 128 rows (0 to 127, 128 to 255, ...) at most 16 rows name the same one
- gate_proj: bfloat16 [32, 2048, 2816], P('sp', None, 'tp'), may hold values from -0.125 to 0.125
- up_proj: bfloat16 [32, 2048, 2816], P('sp', None, 'tp'), may hold values from -0.125 to 0.125
- down_proj: bfloat16 [32, 2816, 2048], P('sp', 'tp'), may hold values from -0.109375 to 0.109375
- out_proj: bfloat16 [2048, 2048], P(None, 'tp'), may hold values from -0.125 to 0.125
- conv_out: bfloat16 [4096, 2048], P('sp', 'tp'), may hold values from -6 to 6
- gate_b: bfloat16 [4096, 2048], P('sp', 'tp'), may hold values from -6 to 6
- gate_c: bfloat16 [4096, 2048], P('sp', 'tp'), may hold values from -6 to 6
- value_v: bfloat16 [4096, 2048], P('sp', 'tp'), may hold values from -6 to 6
- conv_taps: float32 [3, 2048], P(None, 'tp'), may hold values from -3 to 3
Outputs:
- grad_gate: bfloat16 [32, 2048, 2816], P('sp', None, 'tp')
- grad_up: bfloat16 [32, 2048, 2816], P('sp', None, 'tp')
- grad_down: bfloat16 [32, 2816, 2048], P('sp', 'tp')
- grad_out: float32 [2048, 2048], P('sp', 'tp')
- grad_b: bfloat16 [4096, 2048], P('sp', 'tp')
- grad_c: bfloat16 [4096, 2048], P('sp', 'tp')
- grad_v: bfloat16 [4096, 2048], P('sp', 'tp')
The draws below stay inside these ranges and needn't reach their ends.
Inputs may be any that keep to these rules, and one draw needn't show every extreme that they name: `route_ids`: each row names two different experts; within the 128 rows of one index of sp no expert is named by more than 16 rows, a bound that some block reaches.
All inputs are finite; a program needn't handle non-finite values.
Results may differ from the reference program's by a relative error of at most 0.019.
Values may be sent and summed in bfloat16 or wider, within the bound.
A program may use at most 64 MiB of HBM per device.

```python
import math
import jax
import jax.numpy as jnp
import numpy as np
from jax import lax

D = 2048
FF = 2816
TOK_DEV = 128
TOKENS = 4096
EXPERTS = 32
CAP = 16
N_SP = 32
N_TP = 8


def with_spikes(drawn, key, source, target, shards_of, factor):
    owner, partner = [(jnp.arange(drawn.shape[axis_at]) // (drawn.shape[axis_at] // shards_of)).reshape([-1 if axis == axis_at else 1 for axis in range(drawn.ndim)]) for axis_at in (source, target)]
    chosen = jax.random.permutation(key, shards_of)[partner]
    strong = (owner == chosen) | (owner == (partner + shards_of // 2) % shards_of)
    return jnp.where(strong, factor * drawn, drawn)


def block_levels(rng, shape, pieces, smallest, top_value):
    def one(axis_at, blocks):
        heights = jax.random.uniform(jax.random.fold_in(jax.random.fold_in(rng, 6), axis_at), (blocks,), jnp.float32, smallest / len(pieces), top_value / len(pieces))
        return jnp.repeat(jnp.exp(heights), shape[axis_at] // blocks).reshape((-1,) + (1,) * (len(shape) - axis_at - 1))

    level = one(*pieces[0])
    for cut in pieces[1:]:
        level = level * one(*cut)
    return level


def routed_block(key, own, number, rows, amount, top, bound, skew):
    order = jax.random.permutation(key, amount)
    crowded, ordinary = portions_of(amount, rows * top, bound, skew, True), portions_of(amount, rows * top, bound, skew, False)
    places = jnp.arange(amount)

    def named(sizes, rotation):
        used = int((sizes > 0).sum())
        fixed = max(1, used // 4)
        passed = fixed + (places - fixed + rotation * (used - fixed)) % max(1, amount - fixed)
        return jnp.zeros((amount,), jnp.int32).at[order[jnp.where(places < fixed, places, passed)]].set(jnp.asarray(sizes, jnp.int32))

    sizes = jnp.where(number % 4 == 0, named(crowded, number // 4), named(ordinary, number - number // 4 - 1))
    mixed = jax.random.permutation(jax.random.fold_in(own, 3), amount)
    donor, sink = mixed[0:amount // 2 * 2:2], mixed[1:amount // 2 * 2:2]
    room = jnp.minimum(sizes[donor] - 1, bound - sizes[sink]) // 2
    room = jnp.where((donor == order[0]) | (sink == order[0]) | (sizes[sink] == 0), 0, jnp.maximum(room, 0))
    passed = jax.random.randint(jax.random.fold_in(own, 4), (amount // 2,), 0, 1 << 20) % (room + 1)
    sizes = sizes.at[donor].add(-passed).at[sink].add(passed)
    labels = jnp.searchsorted(jnp.cumsum(sizes), jnp.arange(rows * top), side="right").astype(jnp.int32)
    grid = labels.reshape(top, rows).T
    grid = grid[jax.random.permutation(jax.random.fold_in(own, 1), rows)]
    rotation = jax.random.randint(jax.random.fold_in(own, 2), (rows, 1), 0, top)
    return jnp.take_along_axis(grid, (jnp.arange(top)[None, :] + rotation) % top, axis=1)


def portions_of(count, total, most, skew, full):
    weights = [(1 << 20) // math.isqrt(standing ** skew) + 1 for standing in range(1, count + 1)]
    largest = most if full else min(most, max(-(-total // count), total * weights[0] // sum(weights)))
    least = 1 if total - largest >= count - 1 else 0
    given, surplus = [largest] + [least] * (count - 1), total - largest - least * (count - 1)
    while surplus > 0:
        movable = [i for i in range(1, count) if given[i] < largest] or [i for i in range(1, count) if given[i] < most]
        mass, left = sum([weights[i] for i in movable]), surplus
        for i in movable:
            addition = min(most - given[i], max(1, left * weights[i] // mass), surplus)
            given[i] = given[i] + addition
            surplus = surplus - addition
    return np.array(given)


def normal_values(rng, shape, deviation, reach, split=(), kind=jnp.bfloat16):
    loudness = block_levels(rng, shape, split, -0.22, 0.18) if split else 1.0
    values = jax.random.normal(rng, shape, jnp.float32) * deviation * loudness
    return jnp.minimum(jnp.maximum(values, -reach), reach).astype(kind)


def bell_draw_with(rng, extent, spread, limit, pieces, heavy, held_as=jnp.bfloat16):
    array = spread * jax.random.normal(rng, extent, jnp.float32)
    if pieces:
        array = array * block_levels(rng, extent, pieces, -0.22, 0.18)
    return jnp.clip(with_spikes(array, jax.random.fold_in(rng, 3), *heavy), -limit, limit).astype(held_as)


def setup_inputs(seed: int = 0) -> dict:
    arg_keys = jax.random.split(jax.random.key(seed), 14)
    out_grad = bell_draw_with(arg_keys[0], (TOKENS, D), 1.0, 6.0, ((0, 32), (1, 8)), (0, 1, 32, 2.75))
    moe_input = normal_values(arg_keys[1], (TOKENS, D), 1.0, 6.0, ((0, 32), (1, 8)))
    route_weight = jnp.clip(jnp.exp(math.log(1.0) - 1.609438 * jax.random.uniform(arg_keys[2], (TOKENS, 2), jnp.float32) ** block_levels(arg_keys[2], (TOKENS, 2), ((0, 32),), -0.2, 0.2)), 0.2, 1.0)
    route_ids_keys = jax.random.split(jax.random.fold_in(arg_keys[3], 1), TOKENS // TOK_DEV)
    route_ids_turns = jax.random.permutation(jax.random.fold_in(arg_keys[3], 3), TOKENS // TOK_DEV)
    route_ids = jax.vmap(lambda own, number: routed_block(jax.random.fold_in(arg_keys[3], 2), own, number, TOK_DEV, EXPERTS, 2, CAP, 1))(route_ids_keys, route_ids_turns).reshape((TOKENS, 2))
    gate_proj = normal_values(arg_keys[4], (EXPERTS, D, FF), D ** -0.5, 0.125, ((0, 32), (2, 8)))
    up_proj = normal_values(arg_keys[5], (EXPERTS, D, FF), D ** -0.5, 0.125, ((0, 32), (2, 8)))
    down_proj = normal_values(arg_keys[6], (EXPERTS, FF, D), FF ** -0.5, 0.109375, ((0, 32), (1, 8)))
    out_proj = normal_values(arg_keys[7], (D, D), D ** -0.5, 0.125, ((1, 8),))
    conv_out = normal_values(arg_keys[8], (TOKENS, D), 1.0, 6.0, ((0, 32), (1, 8)))
    gate_b = normal_values(arg_keys[9], (TOKENS, D), 1.0, 6.0, ((0, 32), (1, 8)))
    gate_c = normal_values(arg_keys[10], (TOKENS, D), 1.0, 6.0, ((0, 32), (1, 8)))
    value_v = normal_values(arg_keys[11], (TOKENS, D), 1.0, 6.0, ((0, 32), (1, 8)))
    conv_taps = normal_values(arg_keys[12], (3, D), 0.6, 3.0, ((1, 8),), jnp.float32)
    return {"out_grad": out_grad, "moe_input": moe_input, "route_weight": route_weight, "route_ids": route_ids, "gate_proj": gate_proj, "up_proj": up_proj, "down_proj": down_proj, "out_proj": out_proj, "conv_out": conv_out, "gate_b": gate_b, "gate_c": gate_c, "value_v": value_v, "conv_taps": conv_taps}


def slot_table(route_ids):
    flat = route_ids.reshape(N_SP, TOK_DEV * 2).astype(jnp.int32)
    onehot = (flat[:, :, None] == jnp.arange(EXPERTS, dtype=jnp.int32)[None, None, :]).astype(jnp.int32)
    before = jnp.cumsum(onehot, axis=1) - onehot
    slot = jnp.sum(before * onehot, axis=2).astype(jnp.int32)
    return (flat * CAP + slot).astype(jnp.int32)


def place_rows(rows, index):
    return jnp.zeros((EXPERTS * CAP, rows.shape[1]), rows.dtype).at[index].set(rows)


def reference(out_grad, moe_input, route_weight, route_ids, gate_proj, up_proj, down_proj, out_proj, conv_out, gate_b, gate_c, value_v, conv_taps):
    dest = slot_table(route_ids)
    sent = (route_weight[:, :, None] * out_grad.astype(jnp.float32)[:, None, :]).astype(jnp.bfloat16)
    rows_x = jnp.broadcast_to(moe_input[:, None, :], (TOKENS, 2, D)).reshape(N_SP, 2 * TOK_DEV, D)
    rows_dy = sent.reshape(N_SP, 2 * TOK_DEV, D)
    slots_x = jax.vmap(place_rows)(rows_x, dest).reshape(N_SP, EXPERTS, CAP, D)
    slots_dy = jax.vmap(place_rows)(rows_dy, dest).reshape(N_SP, EXPERTS, CAP, D)
    width = FF // N_TP

    def expert(index):
        xin = slots_x[:, index].reshape(N_SP * CAP, D)
        dyin = slots_dy[:, index].reshape(N_SP * CAP, D)
        w_gate = gate_proj[index]
        w_up = up_proj[index]
        w_down = down_proj[index]
        gate = jnp.dot(xin, w_gate, preferred_element_type=jnp.float32)
        upval = jnp.dot(xin, w_up, preferred_element_type=jnp.float32)
        sig = jax.nn.sigmoid(gate)
        act = gate * sig
        hidden = (act * upval).astype(jnp.bfloat16)
        g_down = jnp.dot(hidden.T, dyin, preferred_element_type=jnp.float32).astype(jnp.bfloat16)
        dhid = jnp.dot(dyin, w_down.T, preferred_element_type=jnp.float32)
        dgate = (dhid * upval * (sig * (1.0 + gate * (1.0 - sig)))).astype(jnp.bfloat16)
        dup = (dhid * act).astype(jnp.bfloat16)
        g_gate = jnp.dot(xin.T, dgate, preferred_element_type=jnp.float32).astype(jnp.bfloat16)
        g_up = jnp.dot(xin.T, dup, preferred_element_type=jnp.float32).astype(jnp.bfloat16)
        rows = N_SP * CAP
        part = jnp.einsum('rpf,dpf->prd', dgate.reshape(rows, N_TP, width).astype(jnp.float32),
                          w_gate.reshape(D, N_TP, width).astype(jnp.float32))
        part = part + jnp.einsum('rpf,dpf->prd', dup.reshape(rows, N_TP, width).astype(jnp.float32),
                                 w_up.reshape(D, N_TP, width).astype(jnp.float32))
        part = lax.optimization_barrier(part.astype(jnp.bfloat16)).astype(jnp.float32)
        back = jnp.sum(part, axis=0).astype(jnp.bfloat16)
        return g_gate, g_up, g_down, back

    grad_gate, grad_up, grad_down, backs = lax.map(expert, jnp.arange(EXPERTS, dtype=jnp.int32))
    backs = backs.reshape(EXPERTS, N_SP, CAP, D).transpose(1, 0, 2, 3).reshape(N_SP, EXPERTS * CAP, D)
    picked = jax.vmap(lambda table, index: table[index])(backs, dest)
    moe_grad = jnp.sum(picked.reshape(TOKENS, 2, D).astype(jnp.float32), axis=1)
    grad_h = (out_grad.astype(jnp.float32) + moe_grad).astype(jnp.bfloat16)
    grad_z = jnp.dot(grad_h, out_proj, preferred_element_type=jnp.float32)
    dconv = (grad_z * gate_b.astype(jnp.float32)).astype(jnp.bfloat16)
    grad_b = (grad_z * conv_out.astype(jnp.float32)).astype(jnp.bfloat16)
    padded = jnp.pad(dconv.astype(jnp.float32), ((1, 1), (0, 0)))
    grad_u = conv_taps[0] * padded[2:] + conv_taps[1] * padded[1:-1] + conv_taps[2] * padded[:-2]
    grad_c = (grad_u * value_v.astype(jnp.float32)).astype(jnp.bfloat16)
    grad_v = (grad_u * gate_c.astype(jnp.float32)).astype(jnp.bfloat16)
    mixed = (gate_b.astype(jnp.float32) * conv_out.astype(jnp.float32)).astype(jnp.bfloat16)
    grad_out = jnp.dot(grad_h.T, mixed, preferred_element_type=jnp.float32)
    return grad_gate, grad_up, grad_down, grad_out, grad_b, grad_c, grad_v
```

```python
import functools

import jax
import jax.numpy as jnp
from jax import lax
from jax.experimental import pallas as pl
from jax.experimental.pallas import tpu as pltpu
from jax.sharding import PartitionSpec as P

MESH = pl.DeviceIdType.MESH
NX = 4
HALF = jnp.bfloat16
F32 = jnp.float32
DX = (0, 1, 3, 2)
NT = (((1,), (1,)), ((), ()))
NN = (((1,), (0,)), ((), ()))


def z_order(nz):
    near = [0]
    for d in range(1, nz // 2):
        near += [d, nz - d]
    return tuple(near + [nz // 2])


def remote(src, dst, send_sem, recv_sem, device):
    return pltpu.make_async_remote_copy(
        src_ref=src,
        dst_ref=dst,
        send_sem=send_sem,
        recv_sem=recv_sem,
        device_id=device,
        device_id_type=MESH,
    )


def step_kernel(
    n, q, ids_ref, w_ref, taps_ref, x_hbm, g_hbm, b_hbm, co_hbm, c_hbm, v_hbm, wg_hbm, wu_hbm, wd_hbm, wo_hbm,
    gout_ref, gb_ref, gc_ref, gv_ref, ggate_hbm, gup_hbm, gdown_hbm,
    x_v, g_v, b_v, co_v, c_v, v_v, wgu, wd, wo, p01, p_t, send, buf, mixed,
    hid_t, dgu_t, dgu, po, ps, rsib, pair, ryb, fin, ret, full_h, hx_send, hx, gpart, gr, edge, got, padded, ggate_v, gup_v, gdown_v,
    in_sem, out_sem, s1, r1, sy, ry, ss, rs, smx, rmx, sp, rp, sa, ra, sb, rb, shx, rhx, shy, rhy, shs, rhs,
    sqy, rqy, sqs, rqs, sgz, rgz, se, re,
):
    s, t = lax.axis_index("sp"), lax.axis_index("tp")
    sib = t + 1 - 2 * lax.rem(t, 2)
    z, x = lax.div(s, NX), lax.rem(s, NX)
    nz = n // NX
    ny = q // 2
    zs = z_order(nz)
    tok, cols = x_v.shape
    cap = 4 * tok // n
    total = n * cap
    units = wg_hbm.shape[0]
    high = wd.shape[0]
    share = q * cols // n
    hrows = total // 2

    def sp_at(dz, dx):
        return lax.rem(z + dz + nz, nz) * NX + lax.rem(x + dx + NX, NX)

    def tp_at(d):
        return lax.rem(t + 2 * d + q, q)

    barrier = pltpu.get_barrier_semaphore()
    peers = [(sp_at(dz, dx), t) for dz in zs for dx in DX][1:]
    peers += [(s, tp_at(d)) for d in range(1, ny)] + [(s, sib)]
    for peer in peers:
        pl.semaphore_signal(barrier, inc=1, device_id=peer, device_id_type=MESH)

    loads = [
        pltpu.make_async_copy(source, target, in_sem.at[k])
        for k, (source, target) in enumerate(
            [
                (x_hbm, x_v),
                (g_hbm, g_v),
                (b_hbm, b_v),
                (co_hbm, co_v),
                (wg_hbm, wgu.at[0:units]),
                (wu_hbm, wgu.at[high : high + units]),
                (wd_hbm, wd.at[0:units]),
                (wo_hbm, wo),
                (c_hbm, c_v),
                (v_hbm, v_v),
            ]
        )
    ]
    for load in loads:
        load.start()

    ids0, ids1 = ids_ref[0:1, :], ids_ref[1:2, :]
    experts = lax.broadcasted_iota(jnp.int32, (n, tok), 0)
    named = jnp.logical_or(ids0 == experts, ids1 == experts)
    earlier = jnp.where(
        lax.broadcasted_iota(jnp.int32, (tok, tok), 0) < lax.broadcasted_iota(jnp.int32, (tok, tok), 1), 1.0, 0.0
    )
    before = jnp.dot(
        jnp.where(named, 1.0, 0.0).astype(HALF), earlier.astype(HALF), preferred_element_type=F32
    ).astype(jnp.int32)
    slots = lax.broadcasted_iota(jnp.int32, (cap, tok), 0)
    for e in range(n):
        here = before[e : e + 1, :] == slots
        c0 = jnp.where(jnp.logical_and(here, ids0 == e), 1.0, 0.0)
        c1 = jnp.where(jnp.logical_and(here, ids1 == e), 1.0, 0.0)
        rows = slice(e * cap, (e + 1) * cap)
        p01[rows, 0:tok] = c0.astype(HALF)
        p01[rows, tok : 2 * tok] = c1.astype(HALF)
    loads[0].wait()
    loads[1].wait()
    grad = g_v[...].astype(F32)
    picked = p01[:, 0:tok] + p01[:, tok : 2 * tok]
    send[:, 0] = (
        jnp.dot(picked, x_v[...], preferred_element_type=F32).astype(HALF).reshape(n, cap, cols)
    )
    weighted = []
    for k in range(2):
        wide = jnp.broadcast_to(w_ref[k : k + 1, :], (tok, tok)).T
        wide = jnp.concatenate([wide] * (cols // tok), axis=1)
        weighted.append((wide * grad).astype(HALF))
    send[:, 1] = (
        jnp.dot(p01[...], jnp.concatenate(weighted, axis=0), preferred_element_type=F32)
        .astype(HALF)
        .reshape(n, cap, cols)
    )

    order = [(g, k) for g in range(nz) for k in range(NX)]

    def first(i):
        g, k = order[i]
        e = sp_at(zs[g], DX[k])
        return remote(send.at[e], buf.at[t, g, k], s1.at[i], r1.at[i], (e, t))

    def across(g, way):
        b = buf.at[t, g]
        return remote(b, b, sy.at[g, way], ry.at[g, way], (s, tp_at(1 - 2 * way)))

    def relay(g):
        way = g % 2
        b = buf.at[tp_at(2 * way - 1), g]
        return remote(b, b, sy.at[g, 2], ry.at[g, 2], (s, tp_at(1 - 2 * way)))

    def beside(g, d):
        b = buf.at[tp_at(-d), g]
        return remote(b, b, ss.at[g, d], rs.at[g, d], (s, sib))

    def mixed_x(k):
        return remote(mixed.at[0], mixed.at[k], smx.at[k], rmx.at[k], (sp_at(0, DX[k]), t))

    buf[t, 0, 0] = send[s]
    pl.semaphore_wait(barrier, len(peers))
    for i in range(1, n):
        first(i).start()
    loads[2].wait()
    loads[3].wait()
    mixed[0] = (b_v[...].astype(F32) * co_v[...].astype(F32)).astype(HALF)
    for k in range(1, NX):
        mixed_x(k).start()
    wgu[units:high, :] = jnp.zeros((high - units, q * cols), HALF)
    wgu[high + units : 2 * high, :] = jnp.zeros((high - units, q * cols), HALF)
    wd[units:high, :] = jnp.zeros((high - units, q * cols), HALF)
    p_t[...] = picked.astype(F32).T.astype(HALF)

    def forward(half):
        groups = slice(half * nz // 2, (half + 1) * nz // 2)
        here = slice(half * hrows, (half + 1) * hrows)
        xin = jnp.concatenate([buf[k, groups, :, 0].reshape(hrows, cols) for k in range(q)], axis=1)
        gu = lax.dot_general(wgu[...], xin, NT, preferred_element_type=F32)
        dyin = jnp.concatenate([buf[k, groups, :, 1].reshape(hrows, cols) for k in range(q)], axis=1)
        dhid = lax.dot_general(wd[...], dyin, NT, preferred_element_type=F32)
        gate, upval = gu[0:high], gu[high : 2 * high]
        sig = jax.nn.sigmoid(gate)
        act = gate * sig
        hid_t[:, here] = (act * upval).astype(HALF)
        dgate = dhid * upval * (sig * (1.0 + gate * (1.0 - sig)))
        dup = dhid * act
        dgu_t[0:high, here] = dgate.astype(HALF)
        dgu_t[high : 2 * high, here] = dup.astype(HALF)
        dgu[here, 0:high] = dgate.T.astype(HALF)
        dgu[here, high : 2 * high] = dup.T.astype(HALF)

    def take(g):
        across(g, 0).wait_recv()
        across(g, 1).wait_recv()
        relay(g).start()
        beside(g, 1).start()
        beside(g, ny - 1).start()

    def take_far(g):
        relay(g).wait_recv()
        beside(g, 2).start()

    def drain(g):
        for d in range(ny):
            beside(g, d).wait_recv()

    for g in range(nz):
        for i in range(g * NX, (g + 1) * NX):
            if i:
                first(i).wait_recv()
        across(g, 0).start()
        across(g, 1).start()
        beside(g, 0).start()
        if g >= 1:
            take(g - 1)
        if g >= 2:
            take_far(g - 2)
    for load in loads[4:]:
        load.wait()
    take(nz - 1)
    for g in range(nz // 2):
        drain(g)
    take_far(nz - 2)
    forward(0)
    take_far(nz - 1)
    for g in range(nz // 2, nz):
        drain(g)
    forward(1)

    def part(tt):
        here = pl.ds(pl.multiple_of(tt * cols, cols), cols)
        return jnp.dot(dgu[...], wgu[:, here], preferred_element_type=F32)

    def to_sib(d):
        return remote(ps.at[d], rsib.at[d], sp.at[d], rp.at[d], (s, sib))

    def reduce_y(g, d):
        return remote(pair.at[d, g], ryb.at[d, g], sa.at[g, d], ra.at[g, d], (s, tp_at(d)))

    def back(i):
        g, k = order[i]
        return remote(fin.at[g, k], ret.at[s], sb.at[i], rb.at[i], (sp_at(-zs[g], -DX[k]), t))

    ways = [2, *[d for d in range(1, ny) if d != 2], 0]
    blocks = (nz, NX, cap, cols)
    for d in ways:
        ps[d] = part(lax.rem(sib + 2 * d, q)).astype(HALF).reshape(blocks)
        to_sib(d).start()
    for d in ways:
        po[d] = part(tp_at(d)).astype(HALF).reshape(blocks)
    for d in ways:
        to_sib(d).wait_recv()
    for g in range(nz - 1, -1, -1):
        for d in ways:
            pair[d, g] = (po[d, g].astype(F32) + rsib[d, g].astype(F32)).astype(HALF)
            if d:
                reduce_y(g, d).start()

    def weight_grad(left, low, which, target):
        def step(k, _):
            here = pl.ds(pl.multiple_of(k * cols, cols), cols)
            target[:, here] = jnp.dot(
                left[low : low + units, :],
                buf[k, :, :, which].reshape(total, cols),
                preferred_element_type=F32,
            ).astype(HALF)
            return 0

        lax.fori_loop(0, q, step, 0)

    stores = [
        pltpu.make_async_copy(source, target, out_sem.at[k])
        for k, (source, target) in enumerate(
            [(gdown_v, gdown_hbm), (ggate_v, ggate_hbm), (gup_v, gup_hbm)]
        )
    ]
    weight_grad(hid_t, 0, 1, gdown_v)
    stores[0].start()
    weight_grad(dgu_t, 0, 0, ggate_v)
    stores[1].start()
    for g in range(nz - 1, -1, -1):
        value = pair[0, g].astype(F32)
        for d in range(1, ny):
            reduce_y(g, d).wait_recv()
            value = value + ryb[d, g].astype(F32)
        fin[g] = value.astype(HALF)
        for k in range(NX - 1, -1, -1):
            i = g * NX + k
            if i:
                back(i).start()
            else:
                ret[s] = fin[g, k]
    for i in range(n - 1, 0, -1):
        back(i).wait_recv()

    def h_across(d):
        b = full_h.at[t]
        return remote(b, b, shy.at[d], rhy.at[d], (s, tp_at(d)))

    def h_beside(d):
        b = full_h.at[tp_at(-d)]
        return remote(b, b, shs.at[d], rhs.at[d], (s, sib))

    def exchange(k):
        return remote(
            hx_send.at[lax.rem(x + DX[k], NX)], hx.at[t, k], shx.at[k], rhx.at[k], (sp_at(0, DX[k]), t)
        )

    def q_across(d):
        b = hx.at[t]
        return remote(b, b, sqy.at[d], rqy.at[d], (s, tp_at(d)))

    def q_beside(d):
        b = hx.at[tp_at(-d)]
        return remote(b, b, sqs.at[d], rqs.at[d], (s, sib))

    def term(k):
        zz = lax.rem(z + zs[k], nz)
        return remote(gpart.at[zz], gr.at[k], sgz.at[k], rgz.at[k], (zz * NX + x, t))

    def halo(k):
        there = lax.rem(s + 1, n) if k == 0 else lax.rem(s - 1 + n, n)
        return remote(edge.at[k], got.at[k], se.at[k], re.at[k], (there, t))

    moe = jnp.dot(p_t[...], ret[...].reshape(total, cols), preferred_element_type=F32)
    dh = g_v[...].astype(F32) + moe
    hx_send[...] = dh.T.astype(HALF).reshape(NX, share, tok)
    for k in range(1, NX):
        exchange(k).start()
    full_h[t] = dh.astype(HALF)
    for d in (2, *[d for d in range(1, ny) if d != 2]):
        h_across(d).start()
    h_beside(0).start()
    hx[t, 0] = hx_send[x]
    for k in range(1, NX):
        exchange(k).wait_recv()
    for d in (2, *[d for d in range(1, ny) if d != 2]):
        q_across(d).start()
    q_beside(0).start()
    for d in range(1, ny):
        h_across(d).wait_recv()
        h_beside(d).start()
    for d in range(ny):
        h_beside(d).wait_recv()
    dh_all = jnp.concatenate([full_h[k] for k in range(q)], axis=1)
    grad_z = jnp.dot(dh_all, wo[...], preferred_element_type=F32)
    dconv = (grad_z * b_v[...].astype(F32)).astype(HALF).astype(F32)
    edge[0] = jnp.broadcast_to(dconv[tok - 1 : tok, :], (8, cols))
    edge[1] = jnp.broadcast_to(dconv[0:1, :], (8, cols))
    halo(0).start()
    halo(1).start()
    gb_ref[...] = (grad_z * co_v[...].astype(F32)).astype(HALF)
    padded[8 : 8 + tok, :] = dconv
    for d in range(1, ny):
        q_across(d).wait_recv()
        q_beside(d).start()
    for k in range(1, NX):
        mixed_x(k).wait_recv()
    for d in range(ny):
        q_beside(d).wait_recv()
    left = jnp.concatenate([hx[:, k].reshape(q * share, tok) for k in range(NX)], axis=1)
    out = jnp.dot(left, mixed[...].reshape(NX * tok, cols), preferred_element_type=F32)
    gpart[...] = out.astype(HALF).reshape(nz, share, cols)
    for k in range(nz - 1, 0, -1):
        term(k).start()
    weight_grad(dgu_t, high, 0, gup_v)
    stores[2].start()
    halo(0).wait_recv()
    halo(1).wait_recv()
    padded[0:8, :] = jnp.where(s > 0, got[0], 0.0)
    padded[8 + tok : 16 + tok, :] = jnp.where(s < n - 1, got[1], 0.0)
    grad_u = (
        taps_ref[0:1, :] * padded[9 : 9 + tok, :]
        + taps_ref[1:2, :] * padded[8 : 8 + tok, :]
        + taps_ref[2:3, :] * padded[7 : 7 + tok, :]
    )
    gc_ref[...] = (grad_u * v_v[...].astype(F32)).astype(HALF)
    gv_ref[...] = (grad_u * c_v[...].astype(F32)).astype(HALF)
    sums = gpart[z].astype(F32)
    for k in range(1, nz):
        term(k).wait_recv()
        sums = sums + gr[k].astype(F32)
    gout_ref[...] = sums

    for store in stores:
        store.wait()
    for i in range(1, n):
        first(i).wait_send()
        back(i).wait_send()
    for g in range(nz):
        across(g, 0).wait_send()
        across(g, 1).wait_send()
        relay(g).wait_send()
        for d in range(ny):
            beside(g, d).wait_send()
            if d:
                reduce_y(g, d).wait_send()
    for k in range(1, NX):
        mixed_x(k).wait_send()
        exchange(k).wait_send()
    for d in range(ny):
        to_sib(d).wait_send()
        h_beside(d).wait_send()
        q_beside(d).wait_send()
        if d:
            h_across(d).wait_send()
            q_across(d).wait_send()
    for k in range(1, nz):
        term(k).wait_send()
    halo(0).wait_send()
    halo(1).wait_send()


def store_kernel(*refs):
    count = (len(refs) - 2) // 3
    reads = [pltpu.make_async_copy(refs[k], refs[2 * count + k], refs[-2].at[k]) for k in range(count)]
    writes = [pltpu.make_async_copy(refs[2 * count + k], refs[count + k], refs[-1].at[k]) for k in range(count)]
    for read in reads:
        read.start()
    for read, write in zip(reads, writes):
        read.wait()
        write.start()
    for write in writes:
        write.wait()


def local(
    out_grad,
    moe_input,
    route_weight,
    route_ids,
    gate_proj,
    up_proj,
    down_proj,
    out_proj,
    conv_out,
    gate_b,
    gate_c,
    value_v,
    conv_taps,
):
    n = lax.axis_size("sp")
    q = lax.axis_size("tp")
    tok, cols = moe_input.shape
    width = q * cols
    total = 4 * tok
    cap = total // n
    nz, ny = n // NX, q // 2
    units = down_proj.shape[1]
    high = -(-units // 128) * 128
    share = width // n
    vmem = pl.BlockSpec(memory_space=pltpu.VMEM)
    hbm = pl.BlockSpec(memory_space=pl.ANY)
    dma = pltpu.SemaphoreType.DMA
    blocks = (ny, nz, NX, cap, cols)

    def half(*shape):
        return pltpu.VMEM(shape, HALF)

    sems = [(n,), (nz, 3), (nz, ny), (NX,), (ny,), (nz, ny), (n,), (NX,), (ny,), (ny,), (ny,), (ny,), (nz,), (2,)]
    like = jax.ShapeDtypeStruct((tok, cols), HALF)
    tall = jax.ShapeDtypeStruct((units, width), HALF)
    shapes = (jax.ShapeDtypeStruct((share, cols), F32), like, like, like, tall, tall, tall)
    results = pl.pallas_call(
        functools.partial(step_kernel, n, q),
        out_shape=shapes,
        in_specs=[vmem] * 3 + [hbm] * 10,
        out_specs=(vmem,) * 4 + (hbm,) * 3,
        scratch_shapes=[half(tok, cols)] * 6
        + [
            half(2 * high, width),
            half(high, width),
            half(width, cols),
            half(total, 2 * tok),
            half(tok, total),
            half(n, 2, cap, cols),
            half(q, nz, NX, 2, cap, cols),
            half(NX, tok, cols),
            half(high, total),
            half(2 * high, total),
            half(total, 2 * high),
            half(*blocks),
            half(*blocks),
            half(*blocks),
            half(*blocks),
            half(*blocks),
            half(nz, NX, cap, cols),
            half(n, cap, cols),
            half(q, tok, cols),
            half(NX, share, tok),
            half(q, NX, share, tok),
            half(nz, share, cols),
            half(nz, share, cols),
            pltpu.VMEM((2, 8, cols), F32),
            pltpu.VMEM((2, 8, cols), F32),
            pltpu.VMEM((tok + 16, cols), F32),
            half(units, width),
            half(units, width),
            half(units, width),
            dma((10,)),
            dma((3,)),
        ]
        + [dma(shape) for shape in sems for _ in range(2)],
        compiler_params=pltpu.CompilerParams(
            collective_id=0, has_side_effects=True, vmem_limit_bytes=56 * 2**20
        ),
        name="step",
    )(
        route_ids.T,
        route_weight.T,
        conv_taps,
        moe_input,
        out_grad,
        gate_b,
        conv_out,
        gate_c,
        value_v,
        gate_proj[0].T,
        up_proj[0].T,
        down_proj[0],
        out_proj,
    )
    grad_out, grad_b, grad_c, grad_v, grad_gate, grad_up, grad_down = pl.pallas_call(
        store_kernel,
        out_shape=shapes,
        in_specs=[hbm] * 7,
        out_specs=(hbm,) * 7,
        scratch_shapes=[pltpu.VMEM(shape.shape, shape.dtype) for shape in shapes] + [dma((7,)), dma((7,))],
        name="store",
    )(*results)
    return (grad_gate.T[None], grad_up.T[None], grad_down[None], grad_out, grad_b, grad_c, grad_v)


def solution(mesh):
    in_specs = (
        P("sp", "tp"),
        P("sp", "tp"),
        P("sp", None),
        P("sp", None),
        P("sp", None, "tp"),
        P("sp", None, "tp"),
        P("sp", "tp", None),
        P(None, "tp"),
        P("sp", "tp"),
        P("sp", "tp"),
        P("sp", "tp"),
        P("sp", "tp"),
        P(None, "tp"),
    )
    out_specs = (
        P("sp", None, "tp"),
        P("sp", None, "tp"),
        P("sp", "tp", None),
        P("sp", "tp"),
        P("sp", "tp"),
        P("sp", "tp"),
        P("sp", "tp"),
    )
    return jax.shard_map(local, mesh=mesh, in_specs=in_specs, out_specs=out_specs, check_vma=False)
```

```python
import functools

import jax
import jax.numpy as jnp
from jax import lax
from jax.experimental import pallas as pl
from jax.experimental.pallas import tpu as pltpu
from jax.sharding import PartitionSpec as P

MESH = pl.DeviceIdType.MESH
NX = 4
HALF = jnp.bfloat16
F32 = jnp.float32
DX = (0, 1, 3, 2)
NT = (((1,), (1,)), ((), ()))
NN = (((1,), (0,)), ((), ()))


def z_order(nz):
    near = [0]
    for d in range(1, nz // 2):
        near += [d, nz - d]
    return tuple(near + [nz // 2])


def remote(src, dst, send_sem, recv_sem, device):
    return pltpu.make_async_remote_copy(
        src_ref=src,
        dst_ref=dst,
        send_sem=send_sem,
        recv_sem=recv_sem,
        device_id=device,
        device_id_type=MESH,
    )


def step_kernel(
    n, q, ids_hbm, w_hbm, taps_hbm, x_hbm, g_hbm, b_hbm, co_hbm, c_hbm, v_hbm, wg_hbm, wu_hbm, wd_hbm, wo_hbm,
    gout_ref, gb_ref, gc_ref, gv_ref, ggate_hbm, gup_hbm, gdown_hbm,
    ids_ref, w_ref, taps_ref, x_v, g_v, b_v, co_v, c_v, v_v, wgu, wd, wo, p01, p_t, send, buf, mixed,
    hid_t, dgu_t, dgu, po, ps, rsib, pair, ryb, fin, ret, full_h, hx_send, hx, gpart, gr, edge, got, padded, ggate_v, gup_v, gdown_v,
    in_sem, out_sem, s1, r1, sy, ry, ss, rs, smx, rmx, sp, rp, sa, ra, sb, rb, shx, rhx, shy, rhy, shs, rhs,
    sqs, rqs, sgz, rgz, se, re,
):
    s, t = lax.axis_index("sp"), lax.axis_index("tp")
    sib = t + 1 - 2 * lax.rem(t, 2)
    z, x = lax.div(s, NX), lax.rem(s, NX)
    nz = n // NX
    ny = q // 2
    zs = z_order(nz)
    tok, cols = x_v.shape
    cap = 4 * tok // n
    total = n * cap
    units = wg_hbm.shape[0]
    high = wd.shape[0]
    share = q * cols // n
    hrows = total // 2

    def sp_at(dz, dx):
        return lax.rem(z + dz + nz, nz) * NX + lax.rem(x + dx + NX, NX)

    def tp_at(d):
        return lax.rem(t + 2 * d + q, q)

    pending = []

    def go(copy):
        copy.start()
        pending.append(copy)

    barrier = pltpu.get_barrier_semaphore()
    peers = [(sp_at(dz, dx), t) for dz in zs for dx in DX][:0:-1]
    peers += [(sp_at(0, dx), tp_at(d)) for d in range(1, ny) for dx in DX] + [(s, sib)]
    for peer in peers:
        pl.semaphore_signal(barrier, inc=1, device_id=peer, device_id_type=MESH)

    loads = [
        pltpu.make_async_copy(source, target, in_sem.at[k])
        for k, (source, target) in enumerate(
            [
                (ids_hbm, ids_ref),
                (w_hbm, w_ref),
                (x_hbm, x_v),
                (g_hbm, g_v),
                (b_hbm, b_v),
                (co_hbm, co_v),
                (wg_hbm, wgu.at[0:units]),
                (wu_hbm, wgu.at[high : high + units]),
                (wd_hbm, wd.at[0:units]),
                (wo_hbm, wo),
                (c_hbm, c_v),
                (v_hbm, v_v),
                (taps_hbm, taps_ref),
            ]
        )
    ]
    for load in loads:
        load.start()

    loads[0].wait()
    loads[1].wait()
    ids0, ids1 = ids_ref[0:1, :], ids_ref[1:2, :]
    experts = lax.broadcasted_iota(jnp.int32, (n, tok), 0)
    named = jnp.logical_or(ids0 == experts, ids1 == experts)
    earlier = jnp.where(
        lax.broadcasted_iota(jnp.int32, (tok, tok), 0) < lax.broadcasted_iota(jnp.int32, (tok, tok), 1), 1.0, 0.0
    )
    before = jnp.dot(
        jnp.where(named, 1.0, 0.0).astype(HALF), earlier.astype(HALF), preferred_element_type=F32
    ).astype(jnp.int32)
    slots = lax.broadcasted_iota(jnp.int32, (cap, tok), 0)
    for e in range(n):
        here = before[e : e + 1, :] == slots
        c0 = jnp.where(jnp.logical_and(here, ids0 == e), 1.0, 0.0)
        c1 = jnp.where(jnp.logical_and(here, ids1 == e), 1.0, 0.0)
        rows = slice(e * cap, (e + 1) * cap)
        p01[rows, 0:tok] = c0.astype(HALF)
        p01[rows, tok : 2 * tok] = c1.astype(HALF)
    loads[2].wait()
    loads[3].wait()
    grad = g_v[...].astype(F32)
    picked = p01[:, 0:tok] + p01[:, tok : 2 * tok]
    send[:, 0] = (
        jnp.dot(picked, x_v[...], preferred_element_type=F32).astype(HALF).reshape(n, cap, cols)
    )
    weighted = []
    for k in range(2):
        wide = jnp.broadcast_to(w_ref[k : k + 1, :], (tok, tok)).T
        wide = jnp.concatenate([wide] * (cols // tok), axis=1)
        weighted.append((wide * grad).astype(HALF))
    send[:, 1] = (
        jnp.dot(p01[...], jnp.concatenate(weighted, axis=0), preferred_element_type=F32)
        .astype(HALF)
        .reshape(n, cap, cols)
    )

    order = [(g, k) for g in range(nz) for k in range(NX)]

    def first(i):
        g, k = order[i]
        e = sp_at(zs[g], DX[k])
        return remote(send.at[e], buf.at[t, g, k], s1.at[i], r1.at[i], (e, t))

    def across(g, way):
        b = buf.at[t, g]
        return remote(b, b, sy.at[g, way], ry.at[g, way], (s, tp_at(1 - 2 * way)))

    def relay(g):
        way = g % 2
        b = buf.at[tp_at(2 * way - 1), g]
        return remote(b, b, sy.at[g, 2], ry.at[g, 2], (s, tp_at(1 - 2 * way)))

    def beside(g, d):
        b = buf.at[tp_at(-d), g]
        return remote(b, b, ss.at[g, d], rs.at[g, d], (s, sib))

    def mixed_x(k):
        return remote(mixed.at[0], mixed.at[k], smx.at[k], rmx.at[k], (sp_at(0, DX[k]), t))

    buf[t, 0, 0] = send[s]
    pl.semaphore_wait(barrier, len(peers))
    for i in range(1, n):
        go(first(i))
    loads[4].wait()
    loads[5].wait()
    mixed[0] = (b_v[...].astype(F32) * co_v[...].astype(F32)).astype(HALF)
    for k in range(1, NX):
        go(mixed_x(k))
    wgu[units:high, :] = jnp.zeros((high - units, q * cols), HALF)
    wgu[high + units : 2 * high, :] = jnp.zeros((high - units, q * cols), HALF)
    wd[units:high, :] = jnp.zeros((high - units, q * cols), HALF)
    p_t[...] = picked.astype(F32).T.astype(HALF)

    def forward(half):
        groups = slice(half * nz // 2, (half + 1) * nz // 2)
        here = slice(half * hrows, (half + 1) * hrows)
        xin = jnp.concatenate([buf[k, groups, :, 0].reshape(hrows, cols) for k in range(q)], axis=1)
        gu = lax.dot_general(wgu[...], xin, NT, preferred_element_type=F32)
        dyin = jnp.concatenate([buf[k, groups, :, 1].reshape(hrows, cols) for k in range(q)], axis=1)
        dhid = lax.dot_general(wd[...], dyin, NT, preferred_element_type=F32)
        gate, upval = gu[0:high], gu[high : 2 * high]
        sig = jax.nn.sigmoid(gate)
        act = gate * sig
        hid_t[:, here] = (act * upval).astype(HALF)
        dgate = dhid * upval * (sig * (1.0 + gate * (1.0 - sig)))
        dup = dhid * act
        dgu_t[0:high, here] = dgate.astype(HALF)
        dgu_t[high : 2 * high, here] = dup.astype(HALF)
        dgu[here, 0:high] = dgate.T.astype(HALF)
        dgu[here, high : 2 * high] = dup.T.astype(HALF)

    def gathered(g):
        for i in range(g * NX, (g + 1) * NX):
            if i:
                first(i).wait_recv()
        go(across(g, 0))
        go(across(g, 1))
        go(beside(g, 0))

    def take(g):
        way = g % 2
        across(g, way).wait_recv()
        go(relay(g))
        go(beside(g, 1 if way == 0 else ny - 1))
        across(g, 1 - way).wait_recv()
        go(beside(g, ny - 1 if way == 0 else 1))

    def take_far(g):
        relay(g).wait_recv()
        go(beside(g, 2))

    def drain(g):
        for d in range(ny):
            beside(g, d).wait_recv()

    def part(tt, half):
        here = pl.ds(pl.multiple_of(tt * cols, cols), cols)
        value = jnp.dot(
            dgu[half * hrows : (half + 1) * hrows, :], wgu[:, here], preferred_element_type=F32
        )
        return value.astype(HALF).reshape(nz // 2, NX, cap, cols)

    def groups_of(half):
        return pl.ds(half * nz // 2, nz // 2)

    def to_sib(half, d):
        here = groups_of(half)
        return remote(ps.at[d, here], rsib.at[d, here], sp.at[half, d], rp.at[half, d], (s, sib))

    def reduce_y(g, d):
        return remote(pair.at[d, g], ryb.at[d, g], sa.at[g, d], ra.at[g, d], (s, tp_at(d)))

    def back(i):
        g, k = order[i]
        return remote(fin.at[g, k], ret.at[s], sb.at[i], rb.at[i], (sp_at(-zs[g], -DX[k]), t))

    ways = [2, *[d for d in range(1, ny) if d != 2], 0]

    def partial_sums(half):
        here = slice(half * nz // 2, (half + 1) * nz // 2)
        for d in ways:
            ps[d, here] = part(lax.rem(sib + 2 * d, q), half)
            go(to_sib(half, d))
        for d in ways:
            po[d, here] = part(tp_at(d), half)

    def send_pairs(half):
        for d in ways:
            to_sib(half, d).wait_recv()
        for g in range((half + 1) * nz // 2 - 1, half * nz // 2 - 1, -1):
            for d in ways:
                pair[d, g] = (po[d, g].astype(F32) + rsib[d, g].astype(F32)).astype(HALF)
                if d:
                    go(reduce_y(g, d))

    lead = nz // 2
    for g in range(nz):
        gathered(g)
        if g >= lead - 1:
            take(g - lead + 1)
    for g in range(nz - lead + 1, nz):
        take(g)
        take_far(g - nz + lead - 1)
    take_far(lead - 1)
    for load in loads[6:]:
        load.wait()
    for g in range(lead):
        drain(g)
    forward(0)
    for g in range(lead, nz - 1):
        take_far(g)
    partial_sums(0)
    take_far(nz - 1)
    send_pairs(0)
    for g in range(lead, nz):
        drain(g)
    forward(1)
    partial_sums(1)
    send_pairs(1)

    def weight_grad(left, low, which, target):
        def step(k, _):
            here = pl.ds(pl.multiple_of(k * cols, cols), cols)
            target[:, here] = jnp.dot(
                left[low : low + units, :],
                buf[k, :, :, which].reshape(total, cols),
                preferred_element_type=F32,
            ).astype(HALF)
            return 0

        lax.fori_loop(0, q, step, 0)

    stores = [
        pltpu.make_async_copy(source, target, out_sem.at[k])
        for k, (source, target) in enumerate(
            [(gdown_v, gdown_hbm), (ggate_v, ggate_hbm), (gup_v, gup_hbm)]
        )
    ]
    weight_grad(hid_t, 0, 1, gdown_v)
    stores[0].start()
    weight_grad(dgu_t, 0, 0, ggate_v)
    stores[1].start()
    weight_grad(dgu_t, high, 0, gup_v)
    stores[2].start()
    for g in [*range(lead - 1, -1, -1), *range(nz - 1, lead - 1, -1)]:
        value = pair[0, g].astype(F32)
        for d in range(1, ny):
            reduce_y(g, d).wait_recv()
            value = value + ryb[d, g].astype(F32)
        fin[g] = value.astype(HALF)
        for k in range(NX - 1, -1, -1):
            i = g * NX + k
            if i:
                go(back(i))
            else:
                ret[s] = fin[g, k]
    for i in range(n - 1, 0, -1):
        back(i).wait_recv()

    def h_across(d):
        b = full_h.at[t]
        return remote(b, b, shy.at[d], rhy.at[d], (s, tp_at(d)))

    def h_beside(d):
        b = full_h.at[tp_at(-d)]
        return remote(b, b, shs.at[d], rhs.at[d], (s, sib))

    def exchange(d, k):
        return remote(
            hx_send.at[lax.rem(x + DX[k], NX)],
            hx.at[t, k],
            shx.at[d, k],
            rhx.at[d, k],
            (sp_at(0, DX[k]), tp_at(d)),
        )

    def q_beside(d):
        b = hx.at[tp_at(-d)]
        return remote(b, b, sqs.at[d], rqs.at[d], (s, sib))

    def term(k):
        zz = lax.rem(z + zs[k], nz)
        return remote(gpart.at[zz], gr.at[k], sgz.at[k], rgz.at[k], (zz * NX + x, t))

    def halo(k):
        there = lax.rem(s + 1, n) if k == 0 else lax.rem(s - 1 + n, n)
        return remote(edge.at[k], got.at[k], se.at[k], re.at[k], (there, t))

    moe = jnp.dot(p_t[...], ret[...].reshape(total, cols), preferred_element_type=F32)
    dh = g_v[...].astype(F32) + moe
    hx_send[...] = dh.T.astype(HALF).reshape(NX, share, tok)
    for d in ways:
        for k in range(NX - 1, -1, -1):
            if d or k:
                go(exchange(d, k))
    full_h[t] = dh.astype(HALF)
    for d in ways[:-1]:
        go(h_across(d))
    go(h_beside(0))
    hx[t, 0] = hx_send[x]
    for d in ways[::-1]:
        for k in range(NX):
            if d or k:
                exchange(d, k).wait_recv()
        go(q_beside(d))
    for d in ways[-2::-1]:
        h_across(d).wait_recv()
        go(h_beside(d))
    for k in range(1, NX):
        mixed_x(k).wait_recv()
    for d in ways[::-1]:
        q_beside(d).wait_recv()
    left = jnp.concatenate([hx[:, k].reshape(q * share, tok) for k in range(NX)], axis=1)
    out = jnp.dot(left, mixed[...].reshape(NX * tok, cols), preferred_element_type=F32)
    gpart[...] = out.astype(HALF).reshape(nz, share, cols)
    for k in range(nz - 1, 0, -1):
        go(term(k))
    for d in ways[::-1]:
        h_beside(d).wait_recv()
    dh_all = jnp.concatenate([full_h[k] for k in range(q)], axis=1)
    grad_z = jnp.dot(dh_all, wo[...], preferred_element_type=F32)
    dconv = (grad_z * b_v[...].astype(F32)).astype(HALF).astype(F32)
    edge[0] = jnp.broadcast_to(dconv[tok - 1 : tok, :], (8, cols))
    edge[1] = jnp.broadcast_to(dconv[0:1, :], (8, cols))
    go(halo(0))
    go(halo(1))
    gb_ref[...] = (grad_z * co_v[...].astype(F32)).astype(HALF)
    padded[8 : 8 + tok, :] = dconv
    halo(0).wait_recv()
    halo(1).wait_recv()
    padded[0:8, :] = jnp.where(s > 0, got[0], 0.0)
    padded[8 + tok : 16 + tok, :] = jnp.where(s < n - 1, got[1], 0.0)
    grad_u = (
        taps_ref[0:1, :] * padded[9 : 9 + tok, :]
        + taps_ref[1:2, :] * padded[8 : 8 + tok, :]
        + taps_ref[2:3, :] * padded[7 : 7 + tok, :]
    )
    gc_ref[...] = (grad_u * v_v[...].astype(F32)).astype(HALF)
    gv_ref[...] = (grad_u * c_v[...].astype(F32)).astype(HALF)
    sums = gpart[z].astype(F32)
    for k in range(1, nz):
        term(k).wait_recv()
        sums = sums + gr[k].astype(F32)
    gout_ref[...] = sums

    for store in stores:
        store.wait()
    for copy in pending:
        copy.wait_send()


def store_kernel(*refs):
    count = (len(refs) - 2) // 3
    reads, writes = [], []
    for k in [*range(4, count), *range(4)]:
        held = refs[2 * count + k]
        reads.append(pltpu.make_async_copy(refs[k], held, refs[-2].at[k]))
        writes.append(pltpu.make_async_copy(held, refs[count + k], refs[-1].at[k]))
    for read in reads:
        read.start()
    for read, write in zip(reads, writes):
        read.wait()
        write.start()
    for write in writes:
        write.wait()


def local(
    out_grad,
    moe_input,
    route_weight,
    route_ids,
    gate_proj,
    up_proj,
    down_proj,
    out_proj,
    conv_out,
    gate_b,
    gate_c,
    value_v,
    conv_taps,
):
    n = lax.axis_size("sp")
    q = lax.axis_size("tp")
    tok, cols = moe_input.shape
    width = q * cols
    total = 4 * tok
    cap = total // n
    nz, ny = n // NX, q // 2
    units = down_proj.shape[1]
    high = -(-units // 128) * 128
    share = width // n
    vmem = pl.BlockSpec(memory_space=pltpu.VMEM)
    hbm = pl.BlockSpec(memory_space=pl.ANY)
    dma = pltpu.SemaphoreType.DMA
    blocks = (ny, nz, NX, cap, cols)

    def half(*shape):
        return pltpu.VMEM(shape, HALF)

    sems = [(n,), (nz, 3), (nz, ny), (NX,), (2, ny), (nz, ny), (n,), (ny, NX), (ny,), (ny,), (ny,), (nz,), (2,)]
    like = jax.ShapeDtypeStruct((tok, cols), HALF)
    tall = jax.ShapeDtypeStruct((units, width), HALF)
    shapes = (jax.ShapeDtypeStruct((share, cols), F32), like, like, like, tall, tall, tall)
    results = pl.pallas_call(
        functools.partial(step_kernel, n, q),
        out_shape=shapes,
        in_specs=[hbm] * 13,
        out_specs=(vmem,) * 4 + (hbm,) * 3,
        scratch_shapes=[pltpu.VMEM((2, tok), jnp.int32), pltpu.VMEM((2, tok), F32), pltpu.VMEM((3, cols), F32)]
        + [half(tok, cols)] * 6
        + [
            half(2 * high, width),
            half(high, width),
            half(width, cols),
            half(total, 2 * tok),
            half(tok, total),
            half(n, 2, cap, cols),
            half(q, nz, NX, 2, cap, cols),
            half(NX, tok, cols),
            half(high, total),
            half(2 * high, total),
            half(total, 2 * high),
            half(*blocks),
            half(*blocks),
            half(*blocks),
            half(*blocks),
            half(*blocks),
            half(nz, NX, cap, cols),
            half(n, cap, cols),
            half(q, tok, cols),
            half(NX, share, tok),
            half(q, NX, share, tok),
            half(nz, share, cols),
            half(nz, share, cols),
            pltpu.VMEM((2, 8, cols), F32),
            pltpu.VMEM((2, 8, cols), F32),
            pltpu.VMEM((tok + 16, cols), F32),
            half(units, width),
            half(units, width),
            half(units, width),
            dma((13,)),
            dma((3,)),
        ]
        + [dma(shape) for shape in sems for _ in range(2)],
        compiler_params=pltpu.CompilerParams(
            collective_id=0, has_side_effects=True, vmem_limit_bytes=56 * 2**20
        ),
        name="step",
    )(
        route_ids.T,
        route_weight.T,
        conv_taps,
        moe_input,
        out_grad,
        gate_b,
        conv_out,
        gate_c,
        value_v,
        gate_proj[0].T,
        up_proj[0].T,
        down_proj[0],
        out_proj,
    )
    grad_out, grad_b, grad_c, grad_v, grad_gate, grad_up, grad_down = pl.pallas_call(
        store_kernel,
        out_shape=shapes,
        in_specs=[hbm] * 7,
        out_specs=(hbm,) * 7,
        scratch_shapes=[pltpu.VMEM(shape.shape, shape.dtype) for shape in shapes] + [dma((7,)), dma((7,))],
        name="store",
    )(*results)
    return (grad_gate.T[None], grad_up.T[None], grad_down[None], grad_out, grad_b, grad_c, grad_v)


def solution(mesh):
    in_specs = (
        P("sp", "tp"),
        P("sp", "tp"),
        P("sp", None),
        P("sp", None),
        P("sp", None, "tp"),
        P("sp", None, "tp"),
        P("sp", "tp", None),
        P(None, "tp"),
        P("sp", "tp"),
        P("sp", "tp"),
        P("sp", "tp"),
        P("sp", "tp"),
        P(None, "tp"),
    )
    out_specs = (
        P("sp", None, "tp"),
        P("sp", None, "tp"),
        P("sp", "tp", None),
        P("sp", "tp"),
        P("sp", "tp"),
        P("sp", "tp"),
        P("sp", "tp"),
    )
    return jax.shard_map(local, mesh=mesh, in_specs=in_specs, out_specs=out_specs, check_vma=False)
```

```python
import functools

import jax
import jax.numpy as jnp
from jax import lax
from jax.experimental import pallas as pl
from jax.experimental.pallas import tpu as pltpu
from jax.sharding import PartitionSpec as P

MESH = pl.DeviceIdType.MESH
NX = 4
HALF = jnp.bfloat16
F32 = jnp.float32
DX = (0, 1, 3, 2)
NT = (((1,), (1,)), ((), ()))
NN = (((1,), (0,)), ((), ()))


def z_order(nz):
    near = [0]
    for d in range(1, nz // 2):
        near += [d, nz - d]
    return tuple(near + [nz // 2])


def remote(src, dst, send_sem, recv_sem, device):
    return pltpu.make_async_remote_copy(
        src_ref=src,
        dst_ref=dst,
        send_sem=send_sem,
        recv_sem=recv_sem,
        device_id=device,
        device_id_type=MESH,
    )


def step_kernel(
    n, q, ids_hbm, w_hbm, taps_hbm, x_hbm, g_hbm, b_hbm, co_hbm, c_hbm, v_hbm, wg_hbm, wu_hbm, wd_hbm, wo_hbm,
    gout_ref, gb_ref, gc_ref, gv_ref, ggate_hbm, gup_hbm, gdown_hbm,
    ids_ref, w_ref, taps_ref, x_v, g_v, b_v, co_v, c_v, v_v, wgu, wd, wo, p01, p_t, send, buf, mixed,
    hid_t, dgu_t, dgu, po, ps, rsib, pair, ryb, fin, ret, full_h, hx_send, hx, gpart, gr, edge, got, padded, ggate_v, gup_v, gdown_v,
    in_sem, out_sem, s1, r1, sy, ry, ss, rs, smx, rmx, sp, rp, sa, ra, sb, rb, shx, rhx, shy, rhy, shs, rhs,
    sqs, rqs, sgz, rgz, se, re,
):
    s, t = lax.axis_index("sp"), lax.axis_index("tp")
    sib = t + 1 - 2 * lax.rem(t, 2)
    z, x = lax.div(s, NX), lax.rem(s, NX)
    nz = n // NX
    ny = q // 2
    zs = z_order(nz)
    tok, cols = x_v.shape
    cap = 4 * tok // n
    total = n * cap
    units = wg_hbm.shape[0]
    high = wd.shape[0]
    share = q * cols // n
    hrows = total // 2

    def sp_at(dz, dx):
        return lax.rem(z + dz + nz, nz) * NX + lax.rem(x + dx + NX, NX)

    def tp_at(d):
        return lax.rem(t + 2 * d + q, q)

    pending = []

    def go(copy):
        copy.start()
        pending.append(copy)

    barrier = pltpu.get_barrier_semaphore()
    peers = [(sp_at(dz, dx), t) for dz in zs for dx in DX][:0:-1]
    peers += [(sp_at(0, dx), tp_at(d)) for d in range(1, ny) for dx in DX] + [(s, sib)]
    for peer in peers:
        pl.semaphore_signal(barrier, inc=1, device_id=peer, device_id_type=MESH)

    loads = [
        pltpu.make_async_copy(source, target, in_sem.at[k])
        for k, (source, target) in enumerate(
            [
                (ids_hbm, ids_ref),
                (w_hbm, w_ref),
                (x_hbm, x_v),
                (g_hbm, g_v),
                (b_hbm, b_v),
                (co_hbm, co_v),
                (wg_hbm, wgu.at[0:units]),
                (wu_hbm, wgu.at[high : high + units]),
                (wd_hbm, wd.at[0:units]),
                (wo_hbm, wo),
                (c_hbm, c_v),
                (v_hbm, v_v),
                (taps_hbm, taps_ref),
            ]
        )
    ]
    for load in loads:
        load.start()

    loads[0].wait()
    loads[1].wait()
    ids0, ids1 = ids_ref[0:1, :], ids_ref[1:2, :]
    experts = lax.broadcasted_iota(jnp.int32, (n, tok), 0)
    named = jnp.logical_or(ids0 == experts, ids1 == experts)
    earlier = jnp.where(
        lax.broadcasted_iota(jnp.int32, (tok, tok), 0) < lax.broadcasted_iota(jnp.int32, (tok, tok), 1), 1.0, 0.0
    )
    before = jnp.dot(
        jnp.where(named, 1.0, 0.0).astype(HALF), earlier.astype(HALF), preferred_element_type=F32
    ).astype(jnp.int32)
    slots = lax.broadcasted_iota(jnp.int32, (cap, tok), 0)
    for e in range(n):
        here = before[e : e + 1, :] == slots
        c0 = jnp.where(jnp.logical_and(here, ids0 == e), 1.0, 0.0)
        c1 = jnp.where(jnp.logical_and(here, ids1 == e), 1.0, 0.0)
        rows = slice(e * cap, (e + 1) * cap)
        p01[rows, 0:tok] = c0.astype(HALF)
        p01[rows, tok : 2 * tok] = c1.astype(HALF)
    loads[2].wait()
    loads[3].wait()
    grad = g_v[...].astype(F32)
    picked = p01[:, 0:tok] + p01[:, tok : 2 * tok]
    send[:, 0] = (
        jnp.dot(picked, x_v[...], preferred_element_type=F32).astype(HALF).reshape(n, cap, cols)
    )
    weighted = []
    for k in range(2):
        wide = jnp.broadcast_to(w_ref[k : k + 1, :], (tok, tok)).T
        wide = jnp.concatenate([wide] * (cols // tok), axis=1)
        weighted.append((wide * grad).astype(HALF))
    send[:, 1] = (
        jnp.dot(p01[...], jnp.concatenate(weighted, axis=0), preferred_element_type=F32)
        .astype(HALF)
        .reshape(n, cap, cols)
    )

    order = [(g, k) for g in range(nz) for k in range(NX)]

    def first(i):
        g, k = order[i]
        e = sp_at(zs[g], DX[k])
        return remote(send.at[e], buf.at[t, g, k], s1.at[i], r1.at[i], (e, t))

    def across(g, way):
        b = buf.at[t, g]
        return remote(b, b, sy.at[g, way], ry.at[g, way], (s, tp_at(1 - 2 * way)))

    def relay(g):
        way = g % 2
        b = buf.at[tp_at(2 * way - 1), g]
        return remote(b, b, sy.at[g, 2], ry.at[g, 2], (s, tp_at(1 - 2 * way)))

    def beside(g, d):
        b = buf.at[tp_at(-d), g]
        return remote(b, b, ss.at[g, d], rs.at[g, d], (s, sib))

    def mixed_x(k):
        return remote(mixed.at[0], mixed.at[k], smx.at[k], rmx.at[k], (sp_at(0, DX[k]), t))

    buf[t, 0, 0] = send[s]
    pl.semaphore_wait(barrier, len(peers))
    for i in range(1, n):
        go(first(i))
    loads[4].wait()
    loads[5].wait()
    mixed[0] = (b_v[...].astype(F32) * co_v[...].astype(F32)).astype(HALF)
    for k in range(1, NX):
        go(mixed_x(k))
    wgu[units:high, :] = jnp.zeros((high - units, q * cols), HALF)
    wgu[high + units : 2 * high, :] = jnp.zeros((high - units, q * cols), HALF)
    wd[units:high, :] = jnp.zeros((high - units, q * cols), HALF)
    p_t[...] = picked.astype(F32).T.astype(HALF)

    def forward(half):
        groups = slice(half * nz // 2, (half + 1) * nz // 2)
        here = slice(half * hrows, (half + 1) * hrows)
        xin = jnp.concatenate([buf[k, groups, :, 0].reshape(hrows, cols) for k in range(q)], axis=1)
        gu = lax.dot_general(wgu[...], xin, NT, preferred_element_type=F32)
        dyin = jnp.concatenate([buf[k, groups, :, 1].reshape(hrows, cols) for k in range(q)], axis=1)
        dhid = lax.dot_general(wd[...], dyin, NT, preferred_element_type=F32)
        gate, upval = gu[0:high], gu[high : 2 * high]
        sig = jax.nn.sigmoid(gate)
        act = gate * sig
        hid_t[:, here] = (act * upval).astype(HALF)
        dgate = dhid * upval * (sig * (1.0 + gate * (1.0 - sig)))
        dup = dhid * act
        dgu_t[0:high, here] = dgate.astype(HALF)
        dgu_t[high : 2 * high, here] = dup.astype(HALF)
        dgu[here, 0:high] = dgate.T.astype(HALF)
        dgu[here, high : 2 * high] = dup.T.astype(HALF)

    def gathered(g):
        for i in range(g * NX, (g + 1) * NX):
            if i:
                first(i).wait_recv()
        go(across(g, 0))
        go(across(g, 1))
        go(beside(g, 0))

    def take(g):
        way = g % 2
        across(g, way).wait_recv()
        go(relay(g))
        go(beside(g, 1 if way == 0 else ny - 1))
        across(g, 1 - way).wait_recv()
        go(beside(g, ny - 1 if way == 0 else 1))

    def take_far(g):
        relay(g).wait_recv()
        go(beside(g, 2))

    def drain(g):
        for d in range(ny):
            beside(g, d).wait_recv()

    def part(tt, half):
        here = pl.ds(pl.multiple_of(tt * cols, cols), cols)
        value = jnp.dot(
            dgu[half * hrows : (half + 1) * hrows, :], wgu[:, here], preferred_element_type=F32
        )
        return value.astype(HALF).reshape(nz // 2, NX, cap, cols)

    def groups_of(half):
        return pl.ds(half * nz // 2, nz // 2)

    def to_sib(half, d):
        here = groups_of(half)
        return remote(ps.at[d, here], rsib.at[d, here], sp.at[half, d], rp.at[half, d], (s, sib))

    def reduce_y(g, d):
        return remote(pair.at[d, g], ryb.at[d, g], sa.at[g, d], ra.at[g, d], (s, tp_at(d)))

    def back(i):
        g, k = order[i]
        return remote(fin.at[g, k], ret.at[s], sb.at[i], rb.at[i], (sp_at(-zs[g], -DX[k]), t))

    ways = [2, *[d for d in range(1, ny) if d != 2], 0]

    def partial_sums(half):
        here = slice(half * nz // 2, (half + 1) * nz // 2)
        for d in ways:
            ps[d, here] = part(lax.rem(sib + 2 * d, q), half)
            go(to_sib(half, d))
        for d in ways:
            po[d, here] = part(tp_at(d), half)

    def send_pairs(half):
        for d in ways:
            to_sib(half, d).wait_recv()
        for g in range((half + 1) * nz // 2 - 1, half * nz // 2 - 1, -1):
            for d in ways:
                pair[d, g] = (po[d, g].astype(F32) + rsib[d, g].astype(F32)).astype(HALF)
                if d:
                    go(reduce_y(g, d))

    lead = nz // 2
    for g in range(nz):
        gathered(g)
        if g >= lead - 1:
            take(g - lead + 1)
    for g in range(nz - lead + 1, nz):
        take(g)
        take_far(g - nz + lead - 1)
    take_far(lead - 1)
    for load in loads[6:]:
        load.wait()
    for g in range(lead):
        drain(g)
    forward(0)
    for g in range(lead, nz - 1):
        take_far(g)
    partial_sums(0)
    take_far(nz - 1)
    send_pairs(0)
    for g in range(lead, nz):
        drain(g)
    forward(1)
    partial_sums(1)
    send_pairs(1)

    def weight_grad(left, low, which, target):
        def step(k, _):
            here = pl.ds(pl.multiple_of(k * cols, cols), cols)
            target[:, here] = jnp.dot(
                left[low : low + units, :],
                buf[k, :, :, which].reshape(total, cols),
                preferred_element_type=F32,
            ).astype(HALF)
            return 0

        lax.fori_loop(0, q, step, 0)

    stores = [
        pltpu.make_async_copy(source, target, out_sem.at[k])
        for k, (source, target) in enumerate(
            [(gdown_v, gdown_hbm), (ggate_v, ggate_hbm), (gup_v, gup_hbm)]
        )
    ]
    weight_grad(hid_t, 0, 1, gdown_v)
    stores[0].start()
    for g in [*range(lead - 1, -1, -1), *range(nz - 1, lead - 1, -1)]:
        value = pair[0, g].astype(F32)
        for d in range(1, ny):
            reduce_y(g, d).wait_recv()
            value = value + ryb[d, g].astype(F32)
        fin[g] = value.astype(HALF)
        for k in range(NX - 1, -1, -1):
            i = g * NX + k
            if i:
                go(back(i))
            else:
                ret[s] = fin[g, k]
    for i in range(n - 1, 0, -1):
        back(i).wait_recv()

    def h_across(d):
        b = full_h.at[t]
        return remote(b, b, shy.at[d], rhy.at[d], (s, tp_at(d)))

    def h_beside(d):
        b = full_h.at[tp_at(-d)]
        return remote(b, b, shs.at[d], rhs.at[d], (s, sib))

    def exchange(d, k):
        return remote(
            hx_send.at[lax.rem(x + DX[k], NX)],
            hx.at[t, k],
            shx.at[d, k],
            rhx.at[d, k],
            (sp_at(0, DX[k]), tp_at(d)),
        )

    def q_beside(d):
        b = hx.at[tp_at(-d)]
        return remote(b, b, sqs.at[d], rqs.at[d], (s, sib))

    def term(k):
        zz = lax.rem(z + zs[k], nz)
        return remote(gpart.at[zz], gr.at[k], sgz.at[k], rgz.at[k], (zz * NX + x, t))

    def halo(k):
        there = lax.rem(s + 1, n) if k == 0 else lax.rem(s - 1 + n, n)
        return remote(edge.at[k], got.at[k], se.at[k], re.at[k], (there, t))

    moe = jnp.dot(p_t[...], ret[...].reshape(total, cols), preferred_element_type=F32)
    dh = g_v[...].astype(F32) + moe
    hx_send[...] = dh.T.astype(HALF).reshape(NX, share, tok)
    for d in ways:
        for k in range(NX - 1, -1, -1):
            if d or k:
                go(exchange(d, k))
    full_h[t] = dh.astype(HALF)
    for d in ways[:-1]:
        go(h_across(d))
    go(h_beside(0))
    hx[t, 0] = hx_send[x]
    weight_grad(dgu_t, 0, 0, ggate_v)
    stores[1].start()
    for d in ways[::-1]:
        for k in range(NX):
            if d or k:
                exchange(d, k).wait_recv()
        go(q_beside(d))
    for d in ways[-2::-1]:
        h_across(d).wait_recv()
        go(h_beside(d))
    for k in range(1, NX):
        mixed_x(k).wait_recv()
    for d in ways[::-1]:
        q_beside(d).wait_recv()
    left = jnp.concatenate([hx[:, k].reshape(q * share, tok) for k in range(NX)], axis=1)
    out = jnp.dot(left, mixed[...].reshape(NX * tok, cols), preferred_element_type=F32)
    gpart[...] = out.astype(HALF).reshape(nz, share, cols)
    for k in range(nz - 1, 0, -1):
        go(term(k))
    for d in ways[::-1]:
        h_beside(d).wait_recv()
    dh_all = jnp.concatenate([full_h[k] for k in range(q)], axis=1)
    grad_z = jnp.dot(dh_all, wo[...], preferred_element_type=F32)
    dconv = (grad_z * b_v[...].astype(F32)).astype(HALF).astype(F32)
    edge[0] = jnp.broadcast_to(dconv[tok - 1 : tok, :], (8, cols))
    edge[1] = jnp.broadcast_to(dconv[0:1, :], (8, cols))
    go(halo(0))
    go(halo(1))
    weight_grad(dgu_t, high, 0, gup_v)
    stores[2].start()
    gb_ref[...] = (grad_z * co_v[...].astype(F32)).astype(HALF)
    padded[8 : 8 + tok, :] = dconv
    halo(0).wait_recv()
    halo(1).wait_recv()
    padded[0:8, :] = jnp.where(s > 0, got[0], 0.0)
    padded[8 + tok : 16 + tok, :] = jnp.where(s < n - 1, got[1], 0.0)
    grad_u = (
        taps_ref[0:1, :] * padded[9 : 9 + tok, :]
        + taps_ref[1:2, :] * padded[8 : 8 + tok, :]
        + taps_ref[2:3, :] * padded[7 : 7 + tok, :]
    )
    gc_ref[...] = (grad_u * v_v[...].astype(F32)).astype(HALF)
    gv_ref[...] = (grad_u * c_v[...].astype(F32)).astype(HALF)
    sums = gpart[z].astype(F32)
    for k in range(1, nz):
        term(k).wait_recv()
        sums = sums + gr[k].astype(F32)
    gout_ref[...] = sums

    for store in stores:
        store.wait()
    for copy in pending:
        copy.wait_send()


def store_kernel(*refs):
    count = (len(refs) - 2) // 3
    reads, writes = [], []
    for k in [*range(4, count), *range(4)]:
        held = refs[2 * count + k]
        reads.append(pltpu.make_async_copy(refs[k], held, refs[-2].at[k]))
        writes.append(pltpu.make_async_copy(held, refs[count + k], refs[-1].at[k]))
    for read in reads:
        read.start()
    for read, write in zip(reads, writes):
        read.wait()
        write.start()
    for write in writes:
        write.wait()


def local(
    out_grad,
    moe_input,
    route_weight,
    route_ids,
    gate_proj,
    up_proj,
    down_proj,
    out_proj,
    conv_out,
    gate_b,
    gate_c,
    value_v,
    conv_taps,
):
    n = lax.axis_size("sp")
    q = lax.axis_size("tp")
    tok, cols = moe_input.shape
    width = q * cols
    total = 4 * tok
    cap = total // n
    nz, ny = n // NX, q // 2
    units = down_proj.shape[1]
    high = -(-units // 128) * 128
    share = width // n
    vmem = pl.BlockSpec(memory_space=pltpu.VMEM)
    hbm = pl.BlockSpec(memory_space=pl.ANY)
    dma = pltpu.SemaphoreType.DMA
    blocks = (ny, nz, NX, cap, cols)

    def half(*shape):
        return pltpu.VMEM(shape, HALF)

    sems = [(n,), (nz, 3), (nz, ny), (NX,), (2, ny), (nz, ny), (n,), (ny, NX), (ny,), (ny,), (ny,), (nz,), (2,)]
    like = jax.ShapeDtypeStruct((tok, cols), HALF)
    tall = jax.ShapeDtypeStruct((units, width), HALF)
    shapes = (jax.ShapeDtypeStruct((share, cols), F32), like, like, like, tall, tall, tall)
    results = pl.pallas_call(
        functools.partial(step_kernel, n, q),
        out_shape=shapes,
        in_specs=[hbm] * 13,
        out_specs=(vmem,) * 4 + (hbm,) * 3,
        scratch_shapes=[pltpu.VMEM((2, tok), jnp.int32), pltpu.VMEM((2, tok), F32), pltpu.VMEM((3, cols), F32)]
        + [half(tok, cols)] * 6
        + [
            half(2 * high, width),
            half(high, width),
            half(width, cols),
            half(total, 2 * tok),
            half(tok, total),
            half(n, 2, cap, cols),
            half(q, nz, NX, 2, cap, cols),
            half(NX, tok, cols),
            half(high, total),
            half(2 * high, total),
            half(total, 2 * high),
            half(*blocks),
            half(*blocks),
            half(*blocks),
            half(*blocks),
            half(*blocks),
            half(nz, NX, cap, cols),
            half(n, cap, cols),
            half(q, tok, cols),
            half(NX, share, tok),
            half(q, NX, share, tok),
            half(nz, share, cols),
            half(nz, share, cols),
            pltpu.VMEM((2, 8, cols), F32),
            pltpu.VMEM((2, 8, cols), F32),
            pltpu.VMEM((tok + 16, cols), F32),
            half(units, width),
            half(units, width),
            half(units, width),
            dma((13,)),
            dma((3,)),
        ]
        + [dma(shape) for shape in sems for _ in range(2)],
        compiler_params=pltpu.CompilerParams(
            collective_id=0, has_side_effects=True, vmem_limit_bytes=56 * 2**20
        ),
        name="step",
    )(
        route_ids.T,
        route_weight.T,
        conv_taps,
        moe_input,
        out_grad,
        gate_b,
        conv_out,
        gate_c,
        value_v,
        gate_proj[0].T,
        up_proj[0].T,
        down_proj[0],
        out_proj,
    )
    grad_out, grad_b, grad_c, grad_v, grad_gate, grad_up, grad_down = pl.pallas_call(
        store_kernel,
        out_shape=shapes,
        in_specs=[hbm] * 7,
        out_specs=(hbm,) * 7,
        scratch_shapes=[pltpu.VMEM(shape.shape, shape.dtype) for shape in shapes] + [dma((7,)), dma((7,))],
        name="store",
    )(*results)
    return (grad_gate.T[None], grad_up.T[None], grad_down[None], grad_out, grad_b, grad_c, grad_v)


def solution(mesh):
    in_specs = (
        P("sp", "tp"),
        P("sp", "tp"),
        P("sp", None),
        P("sp", None),
        P("sp", None, "tp"),
        P("sp", None, "tp"),
        P("sp", "tp", None),
        P(None, "tp"),
        P("sp", "tp"),
        P("sp", "tp"),
        P("sp", "tp"),
        P("sp", "tp"),
        P(None, "tp"),
    )
    out_specs = (
        P("sp", None, "tp"),
        P("sp", None, "tp"),
        P("sp", "tp", None),
        P("sp", "tp"),
        P("sp", "tp"),
        P("sp", "tp"),
        P("sp", "tp"),
    )
    return jax.shard_map(local, mesh=mesh, in_specs=in_specs, out_specs=out_specs, check_vma=False)
```

```python
import functools

import jax
import jax.numpy as jnp
from jax import lax
from jax.experimental import pallas as pl
from jax.experimental.pallas import tpu as pltpu
from jax.sharding import PartitionSpec as P

MESH = pl.DeviceIdType.MESH
NX = 4
HALF = jnp.bfloat16
F32 = jnp.float32
DX = (0, 1, 3, 2)
NT = (((1,), (1,)), ((), ()))
NN = (((1,), (0,)), ((), ()))


def z_order(nz):
    near = [0]
    for d in range(1, nz // 2):
        near += [d, nz - d]
    return tuple(near + [nz // 2])


def remote(src, dst, send_sem, recv_sem, device):
    return pltpu.make_async_remote_copy(
        src_ref=src,
        dst_ref=dst,
        send_sem=send_sem,
        recv_sem=recv_sem,
        device_id=device,
        device_id_type=MESH,
    )


def step_kernel(
    n, q, ids_hbm, w_hbm, taps_hbm, x_hbm, g_hbm, b_hbm, co_hbm, c_hbm, v_hbm, wg_hbm, wu_hbm, wd_hbm, wo_hbm,
    gout_ref, gb_ref, gc_ref, gv_ref, ggate_hbm, gup_hbm, gdown_hbm,
    ids_ref, w_ref, taps_ref, x_v, g_v, b_v, co_v, c_v, v_v, wgu, wd, wo, p01, p_t, send, buf, mixed,
    hid_t, dgu_t, dgu, po, ps, rsib, pair, ryb, fin, ret, full_h, hx_send, hx, gpart, gr, edge, got, padded, ggate_v, gup_v, gdown_v,
    in_sem, out_sem, s1, r1, sy, ry, ss, rs, smx, rmx, sp, rp, sa, ra, sb, rb, shx, rhx, shy, rhy, shs, rhs,
    sqs, rqs, sgz, rgz, se, re,
):
    s, t = lax.axis_index("sp"), lax.axis_index("tp")
    sib = t + 1 - 2 * lax.rem(t, 2)
    z, x = lax.div(s, NX), lax.rem(s, NX)
    nz = n // NX
    ny = q // 2
    zs = z_order(nz)
    tok, cols = x_v.shape
    cap = 4 * tok // n
    total = n * cap
    units = wg_hbm.shape[0]
    high = wd.shape[0]
    share = q * cols // n
    hrows = total // 2

    def sp_at(dz, dx):
        return lax.rem(z + dz + nz, nz) * NX + lax.rem(x + dx + NX, NX)

    def tp_at(d):
        return lax.rem(t + 2 * d + q, q)

    pending = []

    def go(copy):
        copy.start()
        pending.append(copy)

    barrier = pltpu.get_barrier_semaphore()
    peers = [(sp_at(dz, dx), t) for dz in zs for dx in DX][:0:-1]
    peers += [(sp_at(0, dx), tp_at(d)) for d in range(1, ny) for dx in DX] + [(s, sib)]
    for peer in peers:
        pl.semaphore_signal(barrier, inc=1, device_id=peer, device_id_type=MESH)

    loads = [
        pltpu.make_async_copy(source, target, in_sem.at[k])
        for k, (source, target) in enumerate(
            [
                (ids_hbm, ids_ref),
                (w_hbm, w_ref),
                (x_hbm, x_v),
                (g_hbm, g_v),
                (b_hbm, b_v),
                (co_hbm, co_v),
                (wg_hbm, wgu.at[0:units]),
                (wu_hbm, wgu.at[high : high + units]),
                (wd_hbm, wd.at[0:units]),
                (wo_hbm, wo),
                (c_hbm, c_v),
                (v_hbm, v_v),
                (taps_hbm, taps_ref),
            ]
        )
    ]
    for load in loads:
        load.start()

    loads[0].wait()
    loads[1].wait()
    ids0, ids1 = ids_ref[0:1, :], ids_ref[1:2, :]
    experts = lax.broadcasted_iota(jnp.int32, (n, tok), 0)
    named = jnp.logical_or(ids0 == experts, ids1 == experts)
    earlier = jnp.where(
        lax.broadcasted_iota(jnp.int32, (tok, tok), 0) < lax.broadcasted_iota(jnp.int32, (tok, tok), 1), 1.0, 0.0
    )
    before = jnp.dot(
        jnp.where(named, 1.0, 0.0).astype(HALF), earlier.astype(HALF), preferred_element_type=F32
    ).astype(jnp.int32)
    slots = lax.broadcasted_iota(jnp.int32, (cap, tok), 0)
    for e in range(n):
        here = before[e : e + 1, :] == slots
        c0 = jnp.where(jnp.logical_and(here, ids0 == e), 1.0, 0.0)
        c1 = jnp.where(jnp.logical_and(here, ids1 == e), 1.0, 0.0)
        rows = slice(e * cap, (e + 1) * cap)
        p01[rows, 0:tok] = c0.astype(HALF)
        p01[rows, tok : 2 * tok] = c1.astype(HALF)
    loads[2].wait()
    loads[3].wait()
    grad = g_v[...].astype(F32)
    picked = p01[:, 0:tok] + p01[:, tok : 2 * tok]
    send[:, 0] = (
        jnp.dot(picked, x_v[...], preferred_element_type=F32).astype(HALF).reshape(n, cap, cols)
    )
    weighted = []
    for k in range(2):
        wide = jnp.broadcast_to(w_ref[k : k + 1, :], (tok, tok)).T
        wide = jnp.concatenate([wide] * (cols // tok), axis=1)
        weighted.append((wide * grad).astype(HALF))
    send[:, 1] = (
        jnp.dot(p01[...], jnp.concatenate(weighted, axis=0), preferred_element_type=F32)
        .astype(HALF)
        .reshape(n, cap, cols)
    )

    order = [(g, k) for g in range(nz) for k in range(NX)]

    def first(i):
        g, k = order[i]
        e = sp_at(zs[g], DX[k])
        return remote(send.at[e], buf.at[t, g, k], s1.at[i], r1.at[i], (e, t))

    def across(g, way):
        b = buf.at[t, g]
        return remote(b, b, sy.at[g, way], ry.at[g, way], (s, tp_at(1 - 2 * way)))

    def relay(g):
        way = g % 2
        b = buf.at[tp_at(2 * way - 1), g]
        return remote(b, b, sy.at[g, 2], ry.at[g, 2], (s, tp_at(1 - 2 * way)))

    def beside(g, d):
        b = buf.at[tp_at(-d), g]
        return remote(b, b, ss.at[g, d], rs.at[g, d], (s, sib))

    def mixed_x(k):
        return remote(mixed.at[0], mixed.at[k], smx.at[k], rmx.at[k], (sp_at(0, DX[k]), t))

    buf[t, 0, 0] = send[s]
    pl.semaphore_wait(barrier, len(peers))
    for i in range(1, n):
        go(first(i))
    loads[4].wait()
    loads[5].wait()
    mixed[0] = (b_v[...].astype(F32) * co_v[...].astype(F32)).astype(HALF)
    for k in range(1, NX):
        go(mixed_x(k))
    wgu[units:high, :] = jnp.zeros((high - units, q * cols), HALF)
    wgu[high + units : 2 * high, :] = jnp.zeros((high - units, q * cols), HALF)
    wd[units:high, :] = jnp.zeros((high - units, q * cols), HALF)
    p_t[...] = picked.astype(F32).T.astype(HALF)

    def forward(half):
        groups = slice(half * nz // 2, (half + 1) * nz // 2)
        here = slice(half * hrows, (half + 1) * hrows)
        xin = jnp.concatenate([buf[k, groups, :, 0].reshape(hrows, cols) for k in range(q)], axis=1)
        gu = lax.dot_general(wgu[...], xin, NT, preferred_element_type=F32)
        dyin = jnp.concatenate([buf[k, groups, :, 1].reshape(hrows, cols) for k in range(q)], axis=1)
        dhid = lax.dot_general(wd[...], dyin, NT, preferred_element_type=F32)
        gate, upval = gu[0:high], gu[high : 2 * high]
        sig = jax.nn.sigmoid(gate)
        act = gate * sig
        hid_t[:, here] = (act * upval).astype(HALF)
        dgate = dhid * upval * (sig * (1.0 + gate * (1.0 - sig)))
        dup = dhid * act
        dgu_t[0:high, here] = dgate.astype(HALF)
        dgu_t[high : 2 * high, here] = dup.astype(HALF)
        dgu[here, 0:high] = dgate.T.astype(HALF)
        dgu[here, high : 2 * high] = dup.T.astype(HALF)

    def gathered(g):
        for i in range(g * NX, (g + 1) * NX):
            if i:
                first(i).wait_recv()
        go(across(g, 0))
        go(across(g, 1))
        go(beside(g, 0))

    def take(g):
        way = g % 2
        across(g, way).wait_recv()
        go(relay(g))
        go(beside(g, 1 if way == 0 else ny - 1))
        across(g, 1 - way).wait_recv()
        go(beside(g, ny - 1 if way == 0 else 1))

    def take_far(g):
        relay(g).wait_recv()
        go(beside(g, 2))

    def drain(g):
        for d in range(ny):
            beside(g, d).wait_recv()

    def part(tt, half):
        here = pl.ds(pl.multiple_of(tt * cols, cols), cols)
        value = jnp.dot(
            dgu[half * hrows : (half + 1) * hrows, :], wgu[:, here], preferred_element_type=F32
        )
        return value.astype(HALF).reshape(nz // 2, NX, cap, cols)

    def groups_of(half):
        return pl.ds(half * nz // 2, nz // 2)

    def to_sib(half, d):
        here = groups_of(half)
        return remote(ps.at[d, here], rsib.at[d, here], sp.at[half, d], rp.at[half, d], (s, sib))

    def reduce_y(g, d):
        return remote(pair.at[d, g], ryb.at[d, g], sa.at[g, d], ra.at[g, d], (s, tp_at(d)))

    def back(i):
        g, k = order[i]
        return remote(fin.at[g, k], ret.at[s], sb.at[i], rb.at[i], (sp_at(-zs[g], -DX[k]), t))

    ways = [2, *[d for d in range(1, ny) if d != 2], 0]

    def partial_sums(half):
        here = slice(half * nz // 2, (half + 1) * nz // 2)
        for d in ways:
            ps[d, here] = part(lax.rem(sib + 2 * d, q), half)
            go(to_sib(half, d))
        for d in ways:
            po[d, here] = part(tp_at(d), half)

    def send_pairs(half):
        for d in ways:
            to_sib(half, d).wait_recv()
        for g in range((half + 1) * nz // 2 - 1, half * nz // 2 - 1, -1):
            for d in ways:
                pair[d, g] = (po[d, g].astype(F32) + rsib[d, g].astype(F32)).astype(HALF)
                if d:
                    go(reduce_y(g, d))

    lead = nz // 2
    for g in range(nz):
        gathered(g)
        if g >= lead - 1:
            take(g - lead + 1)
    for g in range(nz - lead + 1, nz):
        take(g)
        take_far(g - nz + lead - 1)
    take_far(lead - 1)
    for load in loads[6:]:
        load.wait()
    for g in range(lead):
        drain(g)
    forward(0)
    for g in range(lead, nz - 1):
        take_far(g)
    partial_sums(0)
    take_far(nz - 1)
    send_pairs(0)
    for g in range(lead, nz):
        drain(g)
    forward(1)
    partial_sums(1)
    send_pairs(1)

    def weight_grad(left, low, which, target):
        def step(k, _):
            here = pl.ds(pl.multiple_of(k * cols, cols), cols)
            target[:, here] = jnp.dot(
                left[low : low + units, :],
                buf[k, :, :, which].reshape(total, cols),
                preferred_element_type=F32,
            ).astype(HALF)
            return 0

        lax.fori_loop(0, q, step, 0)

    stores = [
        pltpu.make_async_copy(source, target, out_sem.at[k])
        for k, (source, target) in enumerate(
            [(gdown_v, gdown_hbm), (ggate_v, ggate_hbm), (gup_v, gup_hbm)]
        )
    ]
    for g in [*range(lead - 1, -1, -1), *range(nz - 1, lead - 1, -1)]:
        value = pair[0, g].astype(F32)
        for d in range(1, ny):
            reduce_y(g, d).wait_recv()
            value = value + ryb[d, g].astype(F32)
        fin[g] = value.astype(HALF)
        for k in range(NX - 1, -1, -1):
            i = g * NX + k
            if i:
                go(back(i))
            else:
                ret[s] = fin[g, k]
    weight_grad(hid_t, 0, 1, gdown_v)
    stores[0].start()
    for i in range(n - 1, 0, -1):
        back(i).wait_recv()

    def h_across(d):
        b = full_h.at[t]
        return remote(b, b, shy.at[d], rhy.at[d], (s, tp_at(d)))

    def h_beside(d):
        b = full_h.at[tp_at(-d)]
        return remote(b, b, shs.at[d], rhs.at[d], (s, sib))

    def exchange(d, k):
        return remote(
            hx_send.at[lax.rem(x + DX[k], NX)],
            hx.at[t, k],
            shx.at[d, k],
            rhx.at[d, k],
            (sp_at(0, DX[k]), tp_at(d)),
        )

    def q_beside(d):
        b = hx.at[tp_at(-d)]
        return remote(b, b, sqs.at[d], rqs.at[d], (s, sib))

    def term(k):
        zz = lax.rem(z + zs[k], nz)
        return remote(gpart.at[k], gr.at[k], sgz.at[k], rgz.at[k], (zz * NX + x, t))

    def halo(k):
        there = lax.rem(s + 1, n) if k == 0 else lax.rem(s - 1 + n, n)
        return remote(edge.at[k], got.at[k], se.at[k], re.at[k], (there, t))

    moe = jnp.dot(p_t[...], ret[...].reshape(total, cols), preferred_element_type=F32)
    dh = g_v[...].astype(F32) + moe
    hx_send[...] = dh.T.astype(HALF).reshape(NX, share, tok)
    for d in ways:
        for k in range(NX - 1, -1, -1):
            if d or k:
                go(exchange(d, k))
    full_h[t] = dh.astype(HALF)
    for d in ways[:-1]:
        go(h_across(d))
    go(h_beside(0))
    hx[t, 0] = hx_send[x]
    weight_grad(dgu_t, 0, 0, ggate_v)
    stores[1].start()
    for d in ways[::-1]:
        for k in range(NX):
            if d or k:
                exchange(d, k).wait_recv()
        go(q_beside(d))
    for d in ways[-2::-1]:
        h_across(d).wait_recv()
        go(h_beside(d))
    for k in range(1, NX):
        mixed_x(k).wait_recv()
    for d in ways[::-1]:
        q_beside(d).wait_recv()
    for low in (nz // 2, 0):
        held = [hx[lax.rem(z + zs[low + j], nz)] for j in range(nz // 2)]
        left = jnp.concatenate(
            [jnp.concatenate([block[k] for k in range(NX)], axis=1) for block in held], axis=0
        )
        out = jnp.dot(left, mixed[...].reshape(NX * tok, cols), preferred_element_type=F32)
        gpart[low : low + nz // 2] = out.astype(HALF).reshape(nz // 2, share, cols)
        for k in range(low + nz // 2 - 1, low - 1, -1):
            if k:
                go(term(k))
    for d in ways[::-1]:
        h_beside(d).wait_recv()
    dh_all = jnp.concatenate([full_h[k] for k in range(q)], axis=1)
    grad_z = jnp.dot(dh_all, wo[...], preferred_element_type=F32)
    dconv = (grad_z * b_v[...].astype(F32)).astype(HALF).astype(F32)
    edge[0] = jnp.broadcast_to(dconv[tok - 1 : tok, :], (8, cols))
    edge[1] = jnp.broadcast_to(dconv[0:1, :], (8, cols))
    go(halo(0))
    go(halo(1))
    weight_grad(dgu_t, high, 0, gup_v)
    stores[2].start()
    gb_ref[...] = (grad_z * co_v[...].astype(F32)).astype(HALF)
    padded[8 : 8 + tok, :] = dconv
    halo(0).wait_recv()
    halo(1).wait_recv()
    padded[0:8, :] = jnp.where(s > 0, got[0], 0.0)
    padded[8 + tok : 16 + tok, :] = jnp.where(s < n - 1, got[1], 0.0)
    grad_u = (
        taps_ref[0:1, :] * padded[9 : 9 + tok, :]
        + taps_ref[1:2, :] * padded[8 : 8 + tok, :]
        + taps_ref[2:3, :] * padded[7 : 7 + tok, :]
    )
    gc_ref[...] = (grad_u * v_v[...].astype(F32)).astype(HALF)
    gv_ref[...] = (grad_u * c_v[...].astype(F32)).astype(HALF)
    sums = gpart[0].astype(F32)
    for k in range(1, nz):
        term(k).wait_recv()
        sums = sums + gr[k].astype(F32)
    gout_ref[...] = sums

    for store in stores:
        store.wait()
    for copy in pending:
        copy.wait_send()


def store_kernel(*refs):
    count = (len(refs) - 2) // 3
    reads, writes = [], []
    for k in [*range(4, count), *range(4)]:
        held = refs[2 * count + k]
        reads.append(pltpu.make_async_copy(refs[k], held, refs[-2].at[k]))
        writes.append(pltpu.make_async_copy(held, refs[count + k], refs[-1].at[k]))
    for read in reads:
        read.start()
    for read, write in zip(reads, writes):
        read.wait()
        write.start()
    for write in writes:
        write.wait()


def local(
    out_grad,
    moe_input,
    route_weight,
    route_ids,
    gate_proj,
    up_proj,
    down_proj,
    out_proj,
    conv_out,
    gate_b,
    gate_c,
    value_v,
    conv_taps,
):
    n = lax.axis_size("sp")
    q = lax.axis_size("tp")
    tok, cols = moe_input.shape
    width = q * cols
    total = 4 * tok
    cap = total // n
    nz, ny = n // NX, q // 2
    units = down_proj.shape[1]
    high = -(-units // 128) * 128
    share = width // n
    vmem = pl.BlockSpec(memory_space=pltpu.VMEM)
    hbm = pl.BlockSpec(memory_space=pl.ANY)
    dma = pltpu.SemaphoreType.DMA
    blocks = (ny, nz, NX, cap, cols)

    def half(*shape):
        return pltpu.VMEM(shape, HALF)

    sems = [(n,), (nz, 3), (nz, ny), (NX,), (2, ny), (nz, ny), (n,), (ny, NX), (ny,), (ny,), (ny,), (nz,), (2,)]
    like = jax.ShapeDtypeStruct((tok, cols), HALF)
    tall = jax.ShapeDtypeStruct((units, width), HALF)
    shapes = (jax.ShapeDtypeStruct((share, cols), F32), like, like, like, tall, tall, tall)
    results = pl.pallas_call(
        functools.partial(step_kernel, n, q),
        out_shape=shapes,
        in_specs=[hbm] * 13,
        out_specs=(vmem,) * 4 + (hbm,) * 3,
        scratch_shapes=[pltpu.VMEM((2, tok), jnp.int32), pltpu.VMEM((2, tok), F32), pltpu.VMEM((3, cols), F32)]
        + [half(tok, cols)] * 6
        + [
            half(2 * high, width),
            half(high, width),
            half(width, cols),
            half(total, 2 * tok),
            half(tok, total),
            half(n, 2, cap, cols),
            half(q, nz, NX, 2, cap, cols),
            half(NX, tok, cols),
            half(high, total),
            half(2 * high, total),
            half(total, 2 * high),
            half(*blocks),
            half(*blocks),
            half(*blocks),
            half(*blocks),
            half(*blocks),
            half(nz, NX, cap, cols),
            half(n, cap, cols),
            half(q, tok, cols),
            half(NX, share, tok),
            half(q, NX, share, tok),
            half(nz, share, cols),
            half(nz, share, cols),
            pltpu.VMEM((2, 8, cols), F32),
            pltpu.VMEM((2, 8, cols), F32),
            pltpu.VMEM((tok + 16, cols), F32),
            half(units, width),
            half(units, width),
            half(units, width),
            dma((13,)),
            dma((3,)),
        ]
        + [dma(shape) for shape in sems for _ in range(2)],
        compiler_params=pltpu.CompilerParams(
            collective_id=0, has_side_effects=True, vmem_limit_bytes=56 * 2**20
        ),
        name="step",
    )(
        route_ids.T,
        route_weight.T,
        conv_taps,
        moe_input,
        out_grad,
        gate_b,
        conv_out,
        gate_c,
        value_v,
        gate_proj[0].T,
        up_proj[0].T,
        down_proj[0],
        out_proj,
    )
    grad_out, grad_b, grad_c, grad_v, grad_gate, grad_up, grad_down = pl.pallas_call(
        store_kernel,
        out_shape=shapes,
        in_specs=[hbm] * 7,
        out_specs=(hbm,) * 7,
        scratch_shapes=[pltpu.VMEM(shape.shape, shape.dtype) for shape in shapes] + [dma((7,)), dma((7,))],
        name="store",
    )(*results)
    return (grad_gate.T[None], grad_up.T[None], grad_down[None], grad_out, grad_b, grad_c, grad_v)


def solution(mesh):
    in_specs = (
        P("sp", "tp"),
        P("sp", "tp"),
        P("sp", None),
        P("sp", None),
        P("sp", None, "tp"),
        P("sp", None, "tp"),
        P("sp", "tp", None),
        P(None, "tp"),
        P("sp", "tp"),
        P("sp", "tp"),
        P("sp", "tp"),
        P("sp", "tp"),
        P(None, "tp"),
    )
    out_specs = (
        P("sp", None, "tp"),
        P("sp", None, "tp"),
        P("sp", "tp", None),
        P("sp", "tp"),
        P("sp", "tp"),
        P("sp", "tp"),
        P("sp", "tp"),
    )
    return jax.shard_map(local, mesh=mesh, in_specs=in_specs, out_specs=out_specs, check_vma=False)
```
